32 devices in a mesh: grp: 2 (over y), fs: 4 (over z), tp: 4 (over x, core).
Axes of the slice: x: 2, y: 2, z: 4, core: 2. Of those that a mesh axis runs over, the one named last changes fastest.
Arguments:
- inputs: bfloat16 [6144, 2048], P(('grp', 'fs'), 'tp'), parts along dimension 0, may hold values from -110 to 110, as said below
- mixer_gain: float32 [2048], replicated, may hold values from 0.1 to 1.9
- query_weight: bfloat16 [2048, 1024], P('fs', 'tp'), may hold values from -0.125 to 0.125
- key_weight: bfloat16 [2048, 1024], P('fs', 'tp'), may hold values from -0.125 to 0.125
- value_weight: bfloat16 [2048, 1024], P('fs', 'tp'), may hold values from -0.125 to 0.125
- gate_weight: bfloat16 [2048, 1024], P('fs', 'tp'), may hold values from -0.125 to 0.125
- head_gain: float32 [1024], P('tp'), may hold values from 0.1 to 1.9
- out_weight: bfloat16 [1024, 2048], P('tp', 'fs'), may hold values from -0.1875 to 0.1875
- channel_gain: float32 [2048], replicated, may hold values from 0.1 to 1.9
- up_weight: bfloat16 [2048, 5632], P('fs', 'tp'), may hold values from -0.125 to 0.125
- switch_weight: bfloat16 [2048, 5632], P('fs', 'tp'), may hold values from -0.125 to 0.125
- filter_up: float32 [3, 5632], P(None, 'tp'), may hold values from -3.5 to 3.5
- filter_switch: float32 [3, 5632], P(None, 'tp'), may hold values from -3.5 to 3.5
- down_weight: bfloat16 [5632, 2048], P('tp', 'fs'), may hold values from -0.078125 to 0.078125
Outputs:
- layer_output: bfloat16 [6144, 2048], P(('grp', 'fs'), 'tp'), parts along dimension 0
The draws below stay inside these ranges and needn't reach their ends.
There are 2 independent parts, one for each index of `grp`. The reference program is written for one: setup_inputs(seed, part) draws one part's arguments, and reference() takes and returns one part's arrays. A program takes and returns all parts, laid end to end along the dimension named above; an argument that names none is the same for every part. Nothing has to cross between parts.
Inputs may be any that keep to these rules, and one draw needn't show every extreme that they name: `inputs`: activations of one part.
All inputs are finite; a program needn't handle non-finite values.
Results may differ from the reference program's by a relative error of at most 0.012.
Values may be sent and summed in bfloat16 or wider, within the bound.
No kernel may reach another device: no remote copies, remote signals or barrier semaphores. Data moves between devices by JAX's collectives and lax.ppermute only.
A program may use at most 64 MiB of HBM per device.

```python
import jax
import jax.numpy as jnp
from jax import lax

D = 2048
HEAD = 128
FF = 5632
KERNEL = 3
TOK_DEV = 768
RET = 1024
TOKENS = 3072
N_FS = 4
N_TP = 4


def draw_inputs(key, part):
    keys_list = jax.random.split(jax.random.fold_in(key, 11), 3)
    trend_line = jnp.log(3.0) * (jnp.arange(D, dtype=jnp.float32) / D - 0.5)
    column_scale = jnp.exp(jax.random.uniform(keys_list[1], (D,), jnp.float32, -1.15, 1.15) + trend_line)
    noise_field = jnp.clip(jax.random.normal(keys_list[0], (TOKENS, D), jnp.float32), -6.0, 6.0)
    row_scale = jnp.exp(jax.random.uniform(keys_list[2], (TOKENS, 1), jnp.float32, -1.15, 1.15))
    return (noise_field * row_scale * column_scale[None, :]).astype(jnp.bfloat16)


def shard_levels(stream_key, shape, cuts, smallest, top_value):
    def one(dim, parts):
        heights = jax.random.uniform(jax.random.fold_in(jax.random.fold_in(stream_key, 6), dim), (parts,), jnp.float32, smallest / len(cuts), top_value / len(cuts))
        return jnp.repeat(jnp.exp(heights), shape[dim] // parts).reshape((-1,) + (1,) * (len(shape) - dim - 1))

    level = one(*cuts[0])
    for cut in cuts[1:]:
        level = level * one(*cut)
    return level


def scatter_about(stream_key, dims, scale, limit, cuts=(), held_as=jnp.bfloat16):
    entries = scale * jax.random.normal(stream_key, dims, jnp.float32)
    if cuts:
        entries = entries * shard_levels(stream_key, dims, cuts, -0.22, 0.18)
    return jnp.clip(entries, -limit, limit).astype(held_as)


def setup_inputs(seed: int = 0, part: int = 0) -> dict:
    keys = jax.random.split(jax.random.key(seed), 15)
    part_splits = jax.random.split(jax.random.fold_in(keys[14], part), 15)
    inputs = draw_inputs(jax.random.fold_in(jax.random.fold_in(keys[14], part), 71), part)
    mixer_gain = jnp.clip(1.0 + 0.18 * jax.random.normal(keys[1], (D,), jnp.float32), 0.1, 1.9)
    query_weight = scatter_about(keys[2], (D, RET), D ** -0.5, 0.125, ((0, 4), (1, 4)))
    key_weight = scatter_about(keys[3], (D, RET), D ** -0.5, 0.125, ((0, 4), (1, 4)))
    value_weight = scatter_about(keys[4], (D, RET), D ** -0.5, 0.125, ((0, 4), (1, 4)))
    gate_weight = scatter_about(keys[5], (D, RET), D ** -0.5, 0.125, ((0, 4), (1, 4)))
    head_gain = jnp.clip(1.0 + 0.18 * jax.random.normal(keys[6], (RET,), jnp.float32), 0.1, 1.9)
    out_weight = scatter_about(keys[7], (RET, D), RET ** -0.5, 0.1875, ((0, 4), (1, 4)))
    channel_gain = jnp.clip(1.0 + 0.18 * jax.random.normal(keys[8], (D,), jnp.float32), 0.1, 1.9)
    up_weight = scatter_about(keys[9], (D, FF), D ** -0.5, 0.125, ((0, 4), (1, 4)))
    switch_weight = scatter_about(keys[10], (D, FF), D ** -0.5, 0.125, ((0, 4), (1, 4)))
    filter_up = scatter_about(keys[11], (KERNEL, FF), KERNEL ** -0.5, 3.5, ((1, 4),), jnp.float32)
    filter_switch = scatter_about(keys[12], (KERNEL, FF), KERNEL ** -0.5, 3.5, ((1, 4),), jnp.float32)
    down_weight = scatter_about(keys[13], (FF, D), FF ** -0.5, 0.078125, ((0, 4), (1, 4)))
    return dict(inputs=inputs, mixer_gain=mixer_gain, query_weight=query_weight, key_weight=key_weight, value_weight=value_weight, gate_weight=gate_weight, head_gain=head_gain, out_weight=out_weight, channel_gain=channel_gain, up_weight=up_weight, switch_weight=switch_weight, filter_up=filter_up, filter_switch=filter_switch, down_weight=down_weight)


epsilon = 1e-06

def row_norm(row_block, gain_vector):
    values = row_block.astype(jnp.float32)
    scaled = values * lax.rsqrt(lax.optimization_barrier(jnp.mean(values * values, axis=-1, keepdims=True)) + epsilon)
    return (scaled * gain_vector.astype(jnp.float32)).astype(jnp.bfloat16)

def rotate(field, positions):
    half_width = field.shape[-1] // 2
    frequency = 10000.0 ** (-jnp.arange(half_width, dtype=jnp.float32) * 2.0 / field.shape[-1])
    angles = positions.astype(jnp.float32)[:, None] * frequency[None, :]
    cosine = jnp.cos(angles)[:, None, :]
    sine_part = jnp.sin(angles)[:, None, :]
    first_half = field[..., :half_width]
    second_half = field[..., half_width:]
    return jnp.concatenate([first_half * cosine - second_half * sine_part, first_half * sine_part + second_half * cosine], axis=-1)

def decays(first_head, count, positions):
    head_ids = (first_head + jnp.arange(count, dtype=jnp.int32)).astype(jnp.float32)
    log_decay = jnp.log1p(-jnp.exp2(-5.0 - head_ids))
    causal = positions[:, None] >= positions[None, :]
    distance = jnp.where(causal, positions[:, None] - positions[None, :], 0).astype(jnp.float32)
    return jnp.where(causal[None], jnp.exp(log_decay[:, None, None] * distance[None]), 0.0)

def retention(query_rows, key_rows, value_rows, gate_rows, gain_vector):
    length = query_rows.shape[0]
    count = query_rows.shape[1] // HEAD
    positions = jnp.arange(length, dtype=jnp.int32)
    query_rot = rotate(query_rows.astype(jnp.float32).reshape(length, count, HEAD), positions).astype(jnp.bfloat16)
    key_rot = rotate(key_rows.astype(jnp.float32).reshape(length, count, HEAD), positions).astype(jnp.bfloat16)
    decay_table = decays(0, count, positions)
    scores = jnp.einsum('thd,shd->hts', query_rot.astype(jnp.float32), key_rot.astype(jnp.float32))
    weights = (scores * HEAD ** (-0.5) * decay_table).astype(jnp.bfloat16)
    values = value_rows.reshape(length, count, HEAD).astype(jnp.float32)
    retained = jnp.einsum('hts,shd->thd', weights.astype(jnp.float32), values)
    normalized = retained * lax.rsqrt(lax.optimization_barrier(jnp.mean(retained * retained, axis=-1, keepdims=True)) + epsilon)
    gated_rows = normalized.reshape(length, count * HEAD) * gain_vector * jax.nn.silu(gate_rows.astype(jnp.float32))
    return gated_rows.astype(jnp.bfloat16)

def causal_conv(row_block, tap_weights, length):
    sequences = row_block.astype(jnp.float32).reshape(-1, length, row_block.shape[1])
    width_taps = tap_weights.shape[0]
    padded = jnp.pad(sequences, ((0, 0), (width_taps - 1, 0), (0, 0)))
    result = jnp.zeros_like(sequences)
    for tap_index in range(width_taps):
        result = result + padded[:, tap_index:tap_index + length] * tap_weights[tap_index].astype(jnp.float32)
    return result.reshape(row_block.shape)

def grouped_sum(left_side, right_side, groups):
    block_width = left_side.shape[1] // groups
    result = jnp.zeros((left_side.shape[0], right_side.shape[1]), jnp.float32)
    for group_index in range(groups):
        lower = group_index * block_width
        part_sum = jnp.dot(left_side[:, lower:lower + block_width], right_side[lower:lower + block_width], preferred_element_type=jnp.float32)
        result = result + lax.optimization_barrier(part_sum.astype(jnp.bfloat16)).astype(jnp.float32)
    return result

def reference(inputs, mixer_gain, query_weight, key_weight, value_weight, gate_weight, head_gain, out_weight, channel_gain, up_weight, switch_weight, filter_up, filter_switch, down_weight):
    normed = row_norm(inputs, mixer_gain)
    projected = [jnp.dot(normed, matrix, preferred_element_type=jnp.float32).astype(jnp.bfloat16) for matrix in (query_weight, key_weight, value_weight, gate_weight)]
    shaped = tuple((block.reshape(N_FS, TOK_DEV, block.shape[1]) for block in projected))

    def one_sequence(pieces):
        return retention(pieces[0], pieces[1], pieces[2], pieces[3], head_gain)
    head_out = lax.map(one_sequence, shaped).reshape(inputs.shape[0], -1)
    mixer_sum = grouped_sum(head_out, out_weight, N_TP)
    mixed_rows = (inputs.astype(jnp.float32) + mixer_sum).astype(jnp.bfloat16)
    channel_normed = row_norm(mixed_rows, channel_gain)
    lifted = jnp.dot(channel_normed, up_weight, preferred_element_type=jnp.float32).astype(jnp.bfloat16)
    switched = jnp.dot(channel_normed, switch_weight, preferred_element_type=jnp.float32).astype(jnp.bfloat16)
    lift_mixed = causal_conv(lifted, filter_up, TOK_DEV)
    switch_mixed = causal_conv(switched, filter_switch, TOK_DEV)
    hidden = (lift_mixed * jax.nn.silu(switch_mixed)).astype(jnp.bfloat16)
    channel_sum = grouped_sum(hidden, down_weight, N_TP)
    return (mixed_rows.astype(jnp.float32) + channel_sum).astype(jnp.bfloat16)
```

```python
import jax
import jax.numpy as jnp
from jax import lax
from jax.sharding import PartitionSpec as P

HEAD = 128


epsilon = 1e-06


def row_norm(row_block, gain_vector):
    values = row_block.astype(jnp.float32)
    scaled = values * lax.rsqrt(jnp.mean(values * values, axis=-1, keepdims=True) + epsilon)
    return (scaled * gain_vector).astype(jnp.bfloat16)


def rotate(field, positions):
    half_width = field.shape[-1] // 2
    frequency = 10000.0 ** (-jnp.arange(half_width, dtype=jnp.float32) * 2.0 / field.shape[-1])
    angles = positions.astype(jnp.float32)[:, None] * frequency[None, :]
    cosine = jnp.cos(angles)[:, None, :]
    sine_part = jnp.sin(angles)[:, None, :]
    first_half = field[..., :half_width]
    second_half = field[..., half_width:]
    return jnp.concatenate(
        [
            first_half * cosine - second_half * sine_part,
            first_half * sine_part + second_half * cosine,
        ],
        axis=-1,
    )


def decays(first_head, count, positions):
    head_ids = (first_head + jnp.arange(count, dtype=jnp.int32)).astype(jnp.float32)
    log_decay = jnp.log1p(-jnp.exp2(-5.0 - head_ids))
    causal = positions[:, None] >= positions[None, :]
    distance = jnp.where(causal, positions[:, None] - positions[None, :], 0).astype(jnp.float32)
    return jnp.where(causal[None], jnp.exp(log_decay[:, None, None] * distance[None]), 0.0)


def retention(query_rows, key_rows, value_rows, gate_rows, gain_vector, first_head):
    length = query_rows.shape[0]
    count = query_rows.shape[1] // HEAD
    positions = jnp.arange(length, dtype=jnp.int32)
    query_rot = rotate(
        query_rows.astype(jnp.float32).reshape(length, count, HEAD), positions
    ).astype(jnp.bfloat16)
    key_rot = rotate(key_rows.astype(jnp.float32).reshape(length, count, HEAD), positions).astype(
        jnp.bfloat16
    )
    decay_table = decays(first_head, count, positions)
    scores = jnp.einsum("thd,shd->hts", query_rot, key_rot, preferred_element_type=jnp.float32)
    weights = (scores * HEAD ** (-0.5) * decay_table).astype(jnp.bfloat16)
    retained = jnp.einsum(
        "hts,shd->thd",
        weights,
        value_rows.reshape(length, count, HEAD),
        preferred_element_type=jnp.float32,
    )
    normalized = retained * lax.rsqrt(
        jnp.mean(retained * retained, axis=-1, keepdims=True) + epsilon
    )
    gated_rows = (
        normalized.reshape(length, count * HEAD)
        * gain_vector
        * jax.nn.silu(gate_rows.astype(jnp.float32))
    )
    return gated_rows.astype(jnp.bfloat16)


def causal_conv(row_block, tap_weights, length):
    sequences = row_block.astype(jnp.float32).reshape(-1, length, row_block.shape[1])
    width_taps = tap_weights.shape[0]
    padded = jnp.pad(sequences, ((0, 0), (width_taps - 1, 0), (0, 0)))
    result = jnp.zeros_like(sequences)
    for tap_index in range(width_taps):
        result = result + padded[:, tap_index : tap_index + length] * tap_weights[tap_index]
    return result.reshape(row_block.shape)


def on_large_slice(
    inputs,
    mixer_gain,
    query_weight,
    key_weight,
    value_weight,
    gate_weight,
    head_gain,
    out_weight,
    channel_gain,
    up_weight,
    switch_weight,
    filter_up,
    filter_switch,
    down_weight,
):
    length = inputs.shape[0]
    rows_whole = lax.all_gather(inputs, "tp", axis=1, tiled=True)
    normed = row_norm(rows_whole, mixer_gain)
    pieces = (
        lax.all_gather(query_weight, "fs", axis=0, tiled=True),
        lax.all_gather(key_weight, "fs", axis=0, tiled=True),
        lax.all_gather(value_weight, "fs", axis=0, tiled=True),
        lax.all_gather(gate_weight, "fs", axis=0, tiled=True),
    )
    columns = normed
    sums = tuple(
        (jnp.dot(columns, matrix, preferred_element_type=jnp.float32) for matrix in pieces)
    )
    query_rows, key_rows, value_rows, gate_rows = [block.astype(jnp.bfloat16) for block in sums]
    local_heads = query_rows.shape[1] // HEAD
    head_out = retention(
        query_rows, key_rows, value_rows, gate_rows, head_gain, lax.axis_index("tp") * local_heads
    )
    partial_value = jnp.dot(
        head_out,
        lax.all_gather(out_weight, "fs", axis=1, tiled=True),
        preferred_element_type=jnp.float32,
    )
    summed = lax.psum_scatter(
        partial_value.astype(jnp.bfloat16), "tp", scatter_dimension=1, tiled=True
    ).astype(jnp.float32)
    mixed_rows = (inputs.astype(jnp.float32) + summed).astype(jnp.bfloat16)
    mixed_whole = lax.all_gather(mixed_rows, "tp", axis=1, tiled=True)
    channel_normed = row_norm(mixed_whole, channel_gain)
    pieces = (
        lax.all_gather(up_weight, "fs", axis=0, tiled=True),
        lax.all_gather(switch_weight, "fs", axis=0, tiled=True),
    )
    columns = channel_normed
    lift_sum = jnp.dot(columns, pieces[0], preferred_element_type=jnp.float32)
    switch_sum = jnp.dot(columns, pieces[1], preferred_element_type=jnp.float32)
    lift_mixed = causal_conv(lift_sum.astype(jnp.bfloat16), filter_up, length)
    switch_mixed = causal_conv(switch_sum.astype(jnp.bfloat16), filter_switch, length)
    hidden = (lift_mixed * jax.nn.silu(switch_mixed)).astype(jnp.bfloat16)
    channel_partial = jnp.dot(
        hidden,
        lax.all_gather(down_weight, "fs", axis=1, tiled=True),
        preferred_element_type=jnp.float32,
    )
    channel_sum = lax.psum_scatter(
        channel_partial.astype(jnp.bfloat16), "tp", scatter_dimension=1, tiled=True
    ).astype(jnp.float32)
    return (mixed_rows.astype(jnp.float32) + channel_sum).astype(jnp.bfloat16)


def shift(values, axis, size, amount):
    return lax.ppermute(values, axis, [(i, (i + amount) % size) for i in range(size)])


def ring_lane(shards, n_grp, n_fs):
    part_id = lax.axis_index("grp")
    rings = []
    last = None
    for shard in shards:
        rows = shard.shape[0] // n_grp
        payload = lax.dynamic_slice_in_dim(shard, part_id * rows, rows, 0)
        ring = []
        for step in range(1, n_fs):
            if last is not None and step == 1:
                payload, rings[-1][-1] = lax.optimization_barrier((payload, last))
            payload = shift(payload, "fs", n_fs, 1)
            ring.append(payload)
        last = payload
        rings.append(ring)
    gathered = []
    for ring in rings:
        pieces = []
        for step, piece in enumerate(ring, start=1):
            pieces.append((step, part_id, piece))
            for other in range(1, n_grp):
                pieces.append(
                    (step, (part_id - other) % n_grp, shift(piece, "grp", n_grp, other))
                )
        gathered.append(pieces)
    return gathered


def stack_rows(shard, pieces, n_fs):
    rows = shard.shape[0]
    place = lax.axis_index("fs")
    whole = jnp.zeros((n_fs * rows, shard.shape[1]), shard.dtype)
    whole = lax.dynamic_update_slice_in_dim(whole, shard, place * rows, 0)
    for step, part, piece in pieces:
        start = ((place - step) % n_fs) * rows + part * piece.shape[0]
        whole = lax.dynamic_update_slice_in_dim(whole, piece, start, 0)
    return whole


def stack_blocks(shards, gathered, n_fs):
    columns = shards[0].shape[1]
    place = lax.axis_index("fs")
    rows = sum(shard.shape[0] for shard in shards)
    whole = jnp.zeros((n_fs, rows, columns), shards[0].dtype)
    top = 0
    for shard, pieces in zip(shards, gathered):
        whole = lax.dynamic_update_slice(whole, shard[None], (place, top, 0))
        for step, part, piece in pieces:
            source = (place - step) % n_fs
            whole = lax.dynamic_update_slice(
                whole, piece[None], (source, top + part * piece.shape[0], 0)
            )
        top += shard.shape[0]
    return whole


def partner(values, n_tp):
    return lax.ppermute(values, "tp", [(i, i ^ 1) for i in range(n_tp)])


def gather_features(block, n_tp):
    width = block.shape[1]
    n_chip = n_tp // 2
    place = lax.axis_index("tp")
    chip, core = place // 2, place % 2
    whole = jnp.zeros((block.shape[0], n_tp * width), block.dtype)
    held = [block]
    for step in range(1, n_chip):
        held.append(shift(held[-1], "tp", n_tp, 2))
    for step, piece in enumerate(held):
        source = 2 * ((chip - step) % n_chip)
        whole = lax.dynamic_update_slice(whole, piece, (0, (source + core) * width))
        whole = lax.dynamic_update_slice(
            whole, partner(piece, n_tp), (0, (source + 1 - core) * width)
        )
    return whole


def scatter_features(left, right, n_tp):
    n_chip = n_tp // 2
    place = lax.axis_index("tp")
    chip, core = place // 2, place % 2

    def product(target):
        matrix = lax.dynamic_index_in_dim(right, target, 0, keepdims=False)
        return jnp.dot(left, matrix, preferred_element_type=jnp.float32)

    received = []
    total = None
    for step in list(range(1, n_chip)) + [0]:
        target = 2 * ((chip + step) % n_chip)
        away = partner(product(target + 1 - core).astype(jnp.bfloat16), n_tp)
        both = product(target + core) + away.astype(jnp.float32)
        if step:
            received.append(shift(both.astype(jnp.bfloat16), "tp", n_tp, 2 * step))
        else:
            total = both
    for piece in received:
        total = total + piece.astype(jnp.float32)
    return total


def layer(n_grp, n_fs, n_tp):
    def on_device(
        inputs,
        mixer_gain,
        query_weight,
        key_weight,
        value_weight,
        gate_weight,
        head_gain,
        out_weight,
        channel_gain,
        up_weight,
        switch_weight,
        filter_up,
        filter_switch,
        down_weight,
    ):
        length = inputs.shape[0]
        query_key = jnp.concatenate([query_weight, key_weight], axis=1)
        value_gate = jnp.concatenate([value_weight, gate_weight], axis=1)
        middle = down_weight.shape[0] // 2
        down_parts = (down_weight[:middle], down_weight[middle:])
        first_lane = (query_key, out_weight, up_weight, down_parts[0])
        second_lane = (value_gate, switch_weight, down_parts[1])
        rows_whole = gather_features(inputs, n_tp)
        got_qk, got_out, got_up, got_down0 = ring_lane(first_lane, n_grp, n_fs)
        got_vg, got_switch, got_down1 = ring_lane(second_lane, n_grp, n_fs)
        normed = row_norm(rows_whole, mixer_gain)
        qk_rows = jnp.dot(
            normed, stack_rows(query_key, got_qk, n_fs), preferred_element_type=jnp.float32
        ).astype(jnp.bfloat16)
        vg_rows = jnp.dot(
            normed, stack_rows(value_gate, got_vg, n_fs), preferred_element_type=jnp.float32
        ).astype(jnp.bfloat16)
        width = query_weight.shape[1]
        local_heads = width // HEAD
        head_out = retention(
            qk_rows[:, :width],
            qk_rows[:, width:],
            vg_rows[:, :width],
            vg_rows[:, width:],
            head_gain,
            lax.axis_index("tp") * local_heads,
        )
        summed = scatter_features(head_out, stack_blocks((out_weight,), (got_out,), n_fs), n_tp)
        mixed_rows = (inputs.astype(jnp.float32) + summed).astype(jnp.bfloat16)
        mixed_whole = gather_features(mixed_rows, n_tp)
        channel_normed = row_norm(mixed_whole, channel_gain)
        lift_sum = jnp.dot(
            channel_normed, stack_rows(up_weight, got_up, n_fs), preferred_element_type=jnp.float32
        )
        switch_sum = jnp.dot(
            channel_normed,
            stack_rows(switch_weight, got_switch, n_fs),
            preferred_element_type=jnp.float32,
        )
        lift_mixed = causal_conv(lift_sum.astype(jnp.bfloat16), filter_up, length)
        switch_mixed = causal_conv(switch_sum.astype(jnp.bfloat16), filter_switch, length)
        hidden = (lift_mixed * jax.nn.silu(switch_mixed)).astype(jnp.bfloat16)
        down_whole = stack_blocks(down_parts, (got_down0, got_down1), n_fs)
        channel_sum = scatter_features(hidden, down_whole, n_tp)
        return (mixed_rows.astype(jnp.float32) + channel_sum).astype(jnp.bfloat16)

    return on_device


def solution(mesh):
    n_grp, n_fs, n_tp = (mesh.shape[axis] for axis in ("grp", "fs", "tp"))
    short = n_fs == n_tp and n_fs <= 4 and n_tp % 2 == 0
    chosen = layer(n_grp, n_fs, n_tp) if short else on_large_slice
    return jax.shard_map(
        chosen,
        mesh=mesh,
        in_specs=(
            P(("grp", "fs"), "tp"),
            P(),
            P("fs", "tp"),
            P("fs", "tp"),
            P("fs", "tp"),
            P("fs", "tp"),
            P("tp"),
            P("tp", "fs"),
            P(),
            P("fs", "tp"),
            P("fs", "tp"),
            P(None, "tp"),
            P(None, "tp"),
            P("tp", "fs"),
        ),
        out_specs=P(("grp", "fs"), "tp"),
        check_vma=False,
    )
```

```python
import jax
import jax.numpy as jnp
from jax import lax
from jax.sharding import PartitionSpec as P

HEAD = 128


epsilon = 1e-06


def row_norm(row_block, gain_vector):
    values = row_block.astype(jnp.float32)
    scaled = values * lax.rsqrt(jnp.mean(values * values, axis=-1, keepdims=True) + epsilon)
    return (scaled * gain_vector).astype(jnp.bfloat16)


def rotate(field, positions):
    half_width = field.shape[-1] // 2
    frequency = 10000.0 ** (-jnp.arange(half_width, dtype=jnp.float32) * 2.0 / field.shape[-1])
    angles = positions.astype(jnp.float32)[:, None] * frequency[None, :]
    cosine = jnp.cos(angles)[:, None, :]
    sine_part = jnp.sin(angles)[:, None, :]
    first_half = field[..., :half_width]
    second_half = field[..., half_width:]
    return jnp.concatenate(
        [
            first_half * cosine - second_half * sine_part,
            first_half * sine_part + second_half * cosine,
        ],
        axis=-1,
    )


def decays(first_head, count, positions):
    head_ids = (first_head + jnp.arange(count, dtype=jnp.int32)).astype(jnp.float32)
    log_decay = jnp.log1p(-jnp.exp2(-5.0 - head_ids))
    causal = positions[:, None] >= positions[None, :]
    distance = jnp.where(causal, positions[:, None] - positions[None, :], 0).astype(jnp.float32)
    return jnp.where(causal[None], jnp.exp(log_decay[:, None, None] * distance[None]), 0.0)


def retention(query_rows, key_rows, value_rows, gate_rows, gain_vector, first_head):
    length = query_rows.shape[0]
    count = query_rows.shape[1] // HEAD
    positions = jnp.arange(length, dtype=jnp.int32)
    query_rot = rotate(
        query_rows.astype(jnp.float32).reshape(length, count, HEAD), positions
    ).astype(jnp.bfloat16)
    key_rot = rotate(key_rows.astype(jnp.float32).reshape(length, count, HEAD), positions).astype(
        jnp.bfloat16
    )
    decay_table = decays(first_head, count, positions)
    scores = jnp.einsum("thd,shd->hts", query_rot, key_rot, preferred_element_type=jnp.float32)
    weights = (scores * HEAD ** (-0.5) * decay_table).astype(jnp.bfloat16)
    retained = jnp.einsum(
        "hts,shd->thd",
        weights,
        value_rows.reshape(length, count, HEAD),
        preferred_element_type=jnp.float32,
    )
    normalized = retained * lax.rsqrt(
        jnp.mean(retained * retained, axis=-1, keepdims=True) + epsilon
    )
    gated_rows = (
        normalized.reshape(length, count * HEAD)
        * gain_vector
        * jax.nn.silu(gate_rows.astype(jnp.float32))
    )
    return gated_rows.astype(jnp.bfloat16)


def causal_conv(row_block, tap_weights, length):
    sequences = row_block.astype(jnp.float32).reshape(-1, length, row_block.shape[1])
    width_taps = tap_weights.shape[0]
    padded = jnp.pad(sequences, ((0, 0), (width_taps - 1, 0), (0, 0)))
    result = jnp.zeros_like(sequences)
    for tap_index in range(width_taps):
        result = result + padded[:, tap_index : tap_index + length] * tap_weights[tap_index]
    return result.reshape(row_block.shape)


def on_large_slice(
    inputs,
    mixer_gain,
    query_weight,
    key_weight,
    value_weight,
    gate_weight,
    head_gain,
    out_weight,
    channel_gain,
    up_weight,
    switch_weight,
    filter_up,
    filter_switch,
    down_weight,
):
    length = inputs.shape[0]
    rows_whole = lax.all_gather(inputs, "tp", axis=1, tiled=True)
    normed = row_norm(rows_whole, mixer_gain)
    pieces = (
        lax.all_gather(query_weight, "fs", axis=0, tiled=True),
        lax.all_gather(key_weight, "fs", axis=0, tiled=True),
        lax.all_gather(value_weight, "fs", axis=0, tiled=True),
        lax.all_gather(gate_weight, "fs", axis=0, tiled=True),
    )
    columns = normed
    sums = tuple(
        (jnp.dot(columns, matrix, preferred_element_type=jnp.float32) for matrix in pieces)
    )
    query_rows, key_rows, value_rows, gate_rows = [block.astype(jnp.bfloat16) for block in sums]
    local_heads = query_rows.shape[1] // HEAD
    head_out = retention(
        query_rows, key_rows, value_rows, gate_rows, head_gain, lax.axis_index("tp") * local_heads
    )
    partial_value = jnp.dot(
        head_out,
        lax.all_gather(out_weight, "fs", axis=1, tiled=True),
        preferred_element_type=jnp.float32,
    )
    summed = lax.psum_scatter(
        partial_value.astype(jnp.bfloat16), "tp", scatter_dimension=1, tiled=True
    ).astype(jnp.float32)
    mixed_rows = (inputs.astype(jnp.float32) + summed).astype(jnp.bfloat16)
    mixed_whole = lax.all_gather(mixed_rows, "tp", axis=1, tiled=True)
    channel_normed = row_norm(mixed_whole, channel_gain)
    pieces = (
        lax.all_gather(up_weight, "fs", axis=0, tiled=True),
        lax.all_gather(switch_weight, "fs", axis=0, tiled=True),
    )
    columns = channel_normed
    lift_sum = jnp.dot(columns, pieces[0], preferred_element_type=jnp.float32)
    switch_sum = jnp.dot(columns, pieces[1], preferred_element_type=jnp.float32)
    lift_mixed = causal_conv(lift_sum.astype(jnp.bfloat16), filter_up, length)
    switch_mixed = causal_conv(switch_sum.astype(jnp.bfloat16), filter_switch, length)
    hidden = (lift_mixed * jax.nn.silu(switch_mixed)).astype(jnp.bfloat16)
    channel_partial = jnp.dot(
        hidden,
        lax.all_gather(down_weight, "fs", axis=1, tiled=True),
        preferred_element_type=jnp.float32,
    )
    channel_sum = lax.psum_scatter(
        channel_partial.astype(jnp.bfloat16), "tp", scatter_dimension=1, tiled=True
    ).astype(jnp.float32)
    return (mixed_rows.astype(jnp.float32) + channel_sum).astype(jnp.bfloat16)


def shift(values, axis, size, amount):
    return lax.ppermute(values, axis, [(i, (i + amount) % size) for i in range(size)])


class Lane:
    def __init__(self, n_grp, n_fs):
        self.n_grp, self.n_fs = n_grp, n_fs
        self.sent = []

    def carry(self, shards, holds=None, until=None):
        part_id = lax.axis_index("grp")
        shards = list(shards)
        if self.sent:
            *shards, self.sent[-1][0] = lax.optimization_barrier((*shards, self.sent[-1][0]))
        rows = shards[0].shape[0] // self.n_grp
        self.payload = jnp.concatenate(
            [lax.dynamic_slice_in_dim(shard, part_id * rows, rows, 0) for shard in shards], axis=1
        )
        first = len(self.sent)
        self.step = 1
        self.more(holds, until)
        return shards, first

    def more(self, holds=None, until=None):
        last = self.n_fs - 1
        until = last if until is None else min(until, last)
        for step in range(self.step, until + 1):
            after = tuple((holds or {}).get(step, ()))
            tied = self.sent[-2][1] if len(self.sent) >= 2 else []
            payload = self.payload
            if tied or after:
                held = lax.optimization_barrier((payload, *tied, *after))
                payload = held[0]
                if tied:
                    self.sent[-2][1] = list(held[1 : 1 + len(tied)])
            payload = shift(payload, "fs", self.n_fs, 1)
            others = [shift(payload, "grp", self.n_grp, k) for k in range(1, self.n_grp)]
            self.sent.append([payload, others])
            self.payload = payload
        self.step = until + 1

    def take(self, handle):
        shards, first = handle
        part_id = lax.axis_index("grp")
        pieces = []
        shards[0], piece = lax.optimization_barrier((shards[0], self.sent[first][0]))
        for step in range(1, self.n_fs):
            mine, others = self.sent[first + step - 1]
            pieces.append((step, part_id, piece if step == 1 else mine))
            for other, value in enumerate(others, start=1):
                pieces.append((step, (part_id - other) % self.n_grp, value))
        return shards, pieces


def times_pieces(blocks, chunks, gathered, n_grp, n_fs):
    shards, pieces = gathered
    place = lax.axis_index("fs")
    mine = lax.dynamic_index_in_dim(blocks, place, 0, keepdims=False)
    total = jnp.concatenate(
        [jnp.dot(mine, shard, preferred_element_type=jnp.float32) for shard in shards], axis=1
    )
    for step, part, piece in pieces:
        index = ((place - step) % n_fs) * n_grp + part
        chunk = lax.dynamic_index_in_dim(chunks, index, 0, keepdims=False)
        total = total + jnp.dot(chunk, piece, preferred_element_type=jnp.float32)
    return total.astype(jnp.bfloat16)


def block_norm(blocks, gain_vector, n_grp):
    values = blocks.astype(jnp.float32)
    count, length, width = blocks.shape
    mean = jnp.sum(values * values, axis=(0, 2), keepdims=True) / (count * width)
    gain = gain_vector.reshape(count, 1, width)
    normed = (values * lax.rsqrt(mean + epsilon) * gain).astype(jnp.bfloat16)
    chunks = normed.reshape(count, length, n_grp, width // n_grp).transpose(0, 2, 1, 3)
    return normed, chunks.reshape(count * n_grp, length, width // n_grp)


def stack_rows(gathered, n_fs):
    (shard,), pieces = gathered
    rows = shard.shape[0]
    place = lax.axis_index("fs")
    whole = jnp.zeros((n_fs * rows, shard.shape[1]), shard.dtype)
    whole, shard = lax.optimization_barrier((whole, shard))
    whole = lax.dynamic_update_slice_in_dim(whole, shard, place * rows, 0)
    for step, part, piece in pieces:
        start = ((place - step) % n_fs) * rows + part * piece.shape[0]
        whole = lax.dynamic_update_slice_in_dim(whole, piece, start, 0)
    return whole


def stack_blocks(gathered, n_fs):
    place = lax.axis_index("fs")
    columns = gathered[0][0][0].shape[1]
    rows = sum(shards[0].shape[0] for shards, _ in gathered)
    whole = jnp.zeros((n_fs, rows, columns), jnp.bfloat16)
    top = 0
    for (shard,), pieces in gathered:
        if top == 0:
            whole, shard = lax.optimization_barrier((whole, shard))
        whole = lax.dynamic_update_slice(whole, shard[None], (place, top, 0))
        for step, part, piece in pieces:
            source = (place - step) % n_fs
            whole = lax.dynamic_update_slice(
                whole, piece[None], (source, top + part * piece.shape[0], 0)
            )
        top += shard.shape[0]
    return whole


def partner(values, n_tp):
    return lax.ppermute(values, "tp", [(i, i ^ 1) for i in range(n_tp)])


def gather_features(block, n_tp, wide):
    n_chip = n_tp // 2
    place = lax.axis_index("tp")
    chip, core = place // 2, place % 2
    width = block.shape[1]
    if wide:
        whole = jnp.zeros((block.shape[0], n_tp * width), block.dtype)
    else:
        whole = jnp.zeros((n_tp,) + block.shape, block.dtype)

    def put(whole, piece, source):
        if wide:
            return lax.dynamic_update_slice(whole, piece, (0, source * width))
        return lax.dynamic_update_slice(whole, piece[None], (source, 0, 0))

    held = [block]
    for step in range(1, n_chip):
        held.append(shift(held[-1], "tp", n_tp, 2))
    for step, piece in enumerate(held):
        source = 2 * ((chip - step) % n_chip)
        whole = put(whole, piece, source + core)
        whole = put(whole, partner(piece, n_tp), source + 1 - core)
    return whole


def scatter_features(left, right, n_tp):
    n_chip = n_tp // 2
    place = lax.axis_index("tp")
    chip, core = place // 2, place % 2

    def product(target):
        matrix = lax.dynamic_index_in_dim(right, target, 0, keepdims=False)
        return jnp.dot(left, matrix, preferred_element_type=jnp.float32)

    received = []
    both = None
    for step in list(range(1, n_chip)) + [0]:
        target = 2 * ((chip + step) % n_chip)
        away = partner(product(target + 1 - core).astype(jnp.bfloat16), n_tp)
        both = product(target + core) + away.astype(jnp.float32)
        if step:
            sent = both.astype(jnp.bfloat16)
            received.append(shift(sent, "tp", n_tp, 2 * step))
    total = both
    for piece in received:
        total = total + piece.astype(jnp.float32)
    return total, sent


def layer(n_grp, n_fs, n_tp):
    def on_device(
        inputs,
        mixer_gain,
        query_weight,
        key_weight,
        value_weight,
        gate_weight,
        head_gain,
        out_weight,
        channel_gain,
        up_weight,
        switch_weight,
        filter_up,
        filter_switch,
        down_weight,
    ):
        length = inputs.shape[0]
        middle = down_weight.shape[0] // 2
        rows_whole = gather_features(inputs, n_tp, False)
        one, two = Lane(n_grp, n_fs), Lane(n_grp, n_fs)
        qk, vg = one.carry((query_weight, key_weight)), two.carry((value_weight, gate_weight))
        out, switch = one.carry((out_weight,)), two.carry((switch_weight,))
        three, four = Lane(n_grp, n_fs), Lane(n_grp, n_fs)
        begin = (one.sent[-1][0],)
        up = one.carry((up_weight,), until=1)
        down = (
            three.carry((down_weight[:middle],), {1: begin}, 1),
            four.carry((down_weight[middle:],), {1: begin}, 1),
        )
        got_qk, got_vg = one.take(qk), two.take(vg)
        blocks, chunks = block_norm(rows_whole, mixer_gain, n_grp)
        qk_rows = times_pieces(blocks, chunks, got_qk, n_grp, n_fs)
        vg_rows = times_pieces(blocks, chunks, got_vg, n_grp, n_fs)
        width = query_weight.shape[1]
        local_heads = width // HEAD
        head_out = retention(
            qk_rows[:, :width],
            qk_rows[:, width:],
            vg_rows[:, :width],
            vg_rows[:, width:],
            head_gain,
            lax.axis_index("tp") * local_heads,
        )
        summed, sent = scatter_features(head_out, stack_blocks((one.take(out),), n_fs), n_tp)
        mixed_rows = (inputs.astype(jnp.float32) + summed).astype(jnp.bfloat16)
        mixed_whole = gather_features(mixed_rows, n_tp, True)
        one.more({2: (sent,), 3: (mixed_rows,)})
        tail = {2: (one.sent[-1][0],)}
        three.more(tail)
        four.more(tail)
        channel_normed = row_norm(mixed_whole, channel_gain)
        lifted = jnp.dot(
            channel_normed, stack_rows(one.take(up), n_fs), preferred_element_type=jnp.float32
        ).astype(jnp.bfloat16)
        switched = jnp.dot(
            channel_normed, stack_rows(two.take(switch), n_fs), preferred_element_type=jnp.float32
        ).astype(jnp.bfloat16)
        lift_mixed = causal_conv(lifted, filter_up, length)
        switch_mixed = causal_conv(switched, filter_switch, length)
        hidden = (lift_mixed * jax.nn.silu(switch_mixed)).astype(jnp.bfloat16)
        down_whole = stack_blocks((three.take(down[0]), four.take(down[1])), n_fs)
        channel_sum, _ = scatter_features(hidden, down_whole, n_tp)
        return (mixed_rows.astype(jnp.float32) + channel_sum).astype(jnp.bfloat16)

    return on_device


def solution(mesh):
    n_grp, n_fs, n_tp = (mesh.shape[axis] for axis in ("grp", "fs", "tp"))
    short = n_fs == n_tp and n_fs <= 4 and n_tp % 2 == 0
    chosen = layer(n_grp, n_fs, n_tp) if short else on_large_slice
    return jax.shard_map(
        chosen,
        mesh=mesh,
        in_specs=(
            P(("grp", "fs"), "tp"),
            P(),
            P("fs", "tp"),
            P("fs", "tp"),
            P("fs", "tp"),
            P("fs", "tp"),
            P("tp"),
            P("tp", "fs"),
            P(),
            P("fs", "tp"),
            P("fs", "tp"),
            P(None, "tp"),
            P(None, "tp"),
            P("tp", "fs"),
        ),
        out_specs=P(("grp", "fs"), "tp"),
        check_vma=False,
    )
```
